32 devices in a mesh: fs: 8 (over z, x), tp: 4 (over y, core).
Axes of the slice: x: 2, y: 2, z: 4, core: 2. Of those that a mesh axis runs over, the one named last changes fastest.
Arguments:
- prompt_rows: bfloat16 [512, 3072], P('tp'), may hold values from -6 to 6
- gate_first: float32 [3072, 8192], P('fs', 'tp'), may hold values from -0.109375 to 0.109375
- up_first: float32 [3072, 8192], P('fs', 'tp'), may hold values from -0.109375 to 0.109375
- down_first: float32 [8192, 3072], P('fs', 'tp'), may hold values from -0.0625 to 0.0625
- gate_second: float32 [3072, 8192], P('fs', 'tp'), may hold values from -0.109375 to 0.109375
- up_second: float32 [3072, 8192], P('fs', 'tp'), may hold values from -0.109375 to 0.109375
- down_second: float32 [8192, 3072], P('fs', 'tp'), may hold values from -0.0625 to 0.0625
- pre_gain_first: float32 [3072], replicated, may hold values from 0.1 to 1.9
- post_gain_first: float32 [3072], replicated, may hold values from 0.1 to 1.9
- pre_gain_second: float32 [3072], replicated, may hold values from 0.1 to 1.9
- post_gain_second: float32 [3072], replicated, may hold values from 0.1 to 1.9
Outputs:
- result_rows: bfloat16 [512, 3072], P('tp')
- gate_first_new: bfloat16 [3072, 8192], P(None, 'fs')
- up_first_new: bfloat16 [3072, 8192], P(None, 'fs')
- down_first_new: bfloat16 [8192, 3072], P('fs')
- gate_second_new: bfloat16 [3072, 8192], P(None, 'fs')
- up_second_new: bfloat16 [3072, 8192], P(None, 'fs')
- down_second_new: bfloat16 [8192, 3072], P('fs')
The draws below stay inside these ranges and needn't reach their ends.
All inputs are finite; a program needn't handle non-finite values.
Results may differ from the reference program's by a relative error of at most 0.0071.
Values may be sent and summed in bfloat16 or wider, within the bound.
A program may use at most 192 MiB of HBM per device.

```python
import jax
import jax.numpy as jnp
from jax import lax

D = 3072
FF = 8192
TOKENS = 512


def block_scale(rng, dims, split, least, top_value):
    loudness = 1.0
    for dim, shards_of in split:
        heights = jax.random.uniform(jax.random.fold_in(jax.random.fold_in(rng, 6), dim), (shards_of,), jnp.float32, least / len(split), top_value / len(split))
        loudness = loudness * jnp.repeat(jnp.exp(heights), dims[dim] // shards_of).reshape((-1,) + (1,) * (len(dims) - 1 - dim))
    return loudness


def gaussian(key, shape, spread, bound, pieces=(), kind=jnp.bfloat16):
    values = spread * jax.random.normal(key, shape, jnp.float32)
    if pieces:
        values = values * block_scale(key, shape, pieces, -0.22, 0.18)
    return jnp.clip(values, -bound, bound).astype(kind)


def setup_inputs(seed: int = 0) -> dict:
    key_list = jax.random.split(jax.random.key(seed), 12)
    prompt_rows = gaussian(key_list[0], (TOKENS, D), 1.0, 6.0, ((0, 4),))
    gate_first = gaussian(key_list[1], (D, FF), D ** -0.5, 0.109375, ((0, 8), (1, 4)), jnp.float32)
    up_first = gaussian(key_list[2], (D, FF), D ** -0.5, 0.109375, ((0, 8), (1, 4)), jnp.float32)
    down_first = gaussian(key_list[3], (FF, D), FF ** -0.5, 0.0625, ((0, 8), (1, 4)), jnp.float32)
    gate_second = gaussian(key_list[4], (D, FF), D ** -0.5, 0.109375, ((0, 8), (1, 4)), jnp.float32)
    up_second = gaussian(key_list[5], (D, FF), D ** -0.5, 0.109375, ((0, 8), (1, 4)), jnp.float32)
    down_second = gaussian(key_list[6], (FF, D), FF ** -0.5, 0.0625, ((0, 8), (1, 4)), jnp.float32)
    pre_gain_first = jnp.clip(1.0 + 0.18 * jax.random.normal(key_list[7], (D,), jnp.float32), 0.1, 1.9)
    post_gain_first = jnp.clip(1.0 + 0.18 * jax.random.normal(key_list[8], (D,), jnp.float32), 0.1, 1.9)
    pre_gain_second = jnp.clip(1.0 + 0.18 * jax.random.normal(key_list[9], (D,), jnp.float32), 0.1, 1.9)
    post_gain_second = jnp.clip(1.0 + 0.18 * jax.random.normal(key_list[10], (D,), jnp.float32), 0.1, 1.9)
    return {"prompt_rows": prompt_rows, "gate_first": gate_first, "up_first": up_first, "down_first": down_first, "gate_second": gate_second, "up_second": up_second, "down_second": down_second, "pre_gain_first": pre_gain_first, "post_gain_first": post_gain_first, "pre_gain_second": pre_gain_second, "post_gain_second": post_gain_second}


EPSILON = 1e-06

def fold_gain(gain, weight):
    return (gain[:, None] * weight).astype(jnp.bfloat16)

def half_step(rows, gate, up, down, post_gain):
    floats = rows.astype(jnp.float32)
    normed = (floats * lax.rsqrt(lax.optimization_barrier(jnp.mean(floats * floats, axis=-1, keepdims=True)) + EPSILON)).astype(jnp.bfloat16)
    gate_pre = jnp.dot(normed, gate, preferred_element_type=jnp.float32)
    up_pre = jnp.dot(normed, up, preferred_element_type=jnp.float32)
    hidden = (jax.nn.silu(gate_pre) * up_pre).astype(jnp.bfloat16)
    branch = jnp.dot(hidden, down, preferred_element_type=jnp.float32)
    scale = lax.rsqrt(lax.optimization_barrier(jnp.mean(branch * branch, axis=-1, keepdims=True)) + EPSILON)
    return (floats + 0.5 * branch * scale * post_gain[None, :]).astype(jnp.bfloat16)

def reference(prompt_rows, gate_first, up_first, down_first, gate_second, up_second, down_second, pre_gain_first, post_gain_first, pre_gain_second, post_gain_second):
    gate_a = fold_gain(pre_gain_first, gate_first)
    up_a = fold_gain(pre_gain_first, up_first)
    down_a = down_first.astype(jnp.bfloat16)
    gate_b = fold_gain(pre_gain_second, gate_second)
    up_b = fold_gain(pre_gain_second, up_second)
    down_b = down_second.astype(jnp.bfloat16)
    middle = half_step(prompt_rows, gate_a, up_a, down_a, post_gain_first)
    result = half_step(middle, gate_b, up_b, down_b, post_gain_second)
    return (result, gate_a, up_a, down_a, gate_b, up_b, down_b)
```

```python
import jax
import jax.numpy as jnp
from jax import lax
from jax.sharding import PartitionSpec as P

EPSILON = 1e-06
BOTH = ("fs", "tp")


def rms_scale(floats):
    return lax.rsqrt(jnp.mean(floats * floats, axis=-1, keepdims=True) + EPSILON)


def hop(x, distance, ntp):
    return lax.ppermute(x, "tp", [(t, t ^ distance) for t in range(ntp)])


def spread(piece, ntp):
    held = [(0, piece)]
    distance = ntp // 2
    while distance:
        held += [(d ^ distance, hop(p, distance, ntp)) for d, p in held]
        distance //= 2
    return held


def exchange_rows(folded, nfs, ntp):
    f, t = lax.axis_index("fs"), lax.axis_index("tp")
    m = nfs // ntp
    height, width = folded.shape[0], folded.shape[1] // m
    out = jnp.zeros((height * nfs, width), folded.dtype)
    for s in range(m):
        column = lax.rem(f // ntp + s, m) * width
        piece = lax.dynamic_slice(folded, (0, column), (height, width))
        pairs = []
        for a in range(nfs):
            for b in range(ntp):
                target = b * m + (a // ntp + s) % m
                pairs.append((a * ntp + b, target * ntp + a % ntp))
        piece = lax.ppermute(piece, BOTH, pairs)
        slot = lax.rem(lax.rem(f, m) - s + m, m)
        for distance, block in spread(piece, ntp):
            start = (slot * ntp + jnp.bitwise_xor(t, distance)) * height
            out = lax.dynamic_update_slice(out, block, (start, 0))
    return out


def gather_columns(rounded, ntp):
    t = lax.axis_index("tp")
    height, width = rounded.shape
    out = jnp.zeros((height, width * ntp), rounded.dtype)
    for distance, block in spread(rounded, ntp):
        out = lax.dynamic_update_slice(out, block, (0, jnp.bitwise_xor(t, distance) * width))
    return out


def finish(rows, total, post_gain):
    return (rows.astype(jnp.float32) + 0.5 * total * rms_scale(total) * post_gain[None, :]).astype(
        jnp.bfloat16
    )


def half_step(rows, gate, up, down, post_gain, nfs):
    floats = rows.astype(jnp.float32)
    normed = (floats * rms_scale(floats)).astype(jnp.bfloat16)
    gate_pre = jnp.dot(normed, gate, preferred_element_type=jnp.float32)
    up_pre = jnp.dot(normed, up, preferred_element_type=jnp.float32)
    hidden = (jax.nn.silu(gate_pre) * up_pre).astype(jnp.bfloat16)
    part = jnp.dot(hidden, down, preferred_element_type=jnp.float32)
    count = rows.shape[0]
    if count % nfs or nfs > 16:
        return finish(rows, lax.psum(part, "fs"), post_gain)
    f = lax.axis_index("fs")
    band = count // nfs

    def band_of(x, g):
        return lax.dynamic_slice_in_dim(x, g * band, band, 0)

    total = band_of(part, f)
    narrow = part.astype(jnp.bfloat16)
    for s in range(1, nfs):
        pairs = [(a, a ^ s) for a in range(nfs)]
        total = total + lax.ppermute(
            band_of(narrow, jnp.bitwise_xor(f, s)), "fs", pairs
        ).astype(jnp.float32)
    done = finish(band_of(rows, f), total, post_gain)
    out = jnp.zeros_like(rows)
    out = lax.dynamic_update_slice(out, done, (f * band, 0))
    for s in range(1, nfs):
        pairs = [(a, a ^ s) for a in range(nfs)]
        out = lax.dynamic_update_slice(
            out, lax.ppermute(done, "fs", pairs), (jnp.bitwise_xor(f, s) * band, 0)
        )
    return out


def exchange_wide(folded):
    wide = lax.all_gather(folded, "tp", axis=1, tiled=True)
    return lax.all_to_all(wide, "fs", split_axis=1, concat_axis=0, tiled=True)


def solution(mesh):
    nfs, ntp = mesh.shape["fs"], mesh.shape["tp"]
    power = ntp & (ntp - 1) == 0 and nfs & (nfs - 1) == 0
    direct = power and nfs % ntp == 0 and nfs // ntp <= 4

    def per_device(
        prompt_rows,
        gate_first,
        up_first,
        down_first,
        gate_second,
        up_second,
        down_second,
        pre_gain_first,
        post_gain_first,
        pre_gain_second,
        post_gain_second,
    ):
        height = gate_first.shape[0]
        start = lax.axis_index("fs") * height

        def fold(gain, weight):
            gain = lax.dynamic_slice_in_dim(gain, start, height, 0)[:, None]
            folded = (gain * weight).astype(jnp.bfloat16)
            if direct:
                return exchange_rows(folded, nfs, ntp)
            return exchange_wide(folded)

        def gather(weight):
            rounded = weight.astype(jnp.bfloat16)
            if power:
                return gather_columns(rounded, ntp)
            return lax.all_gather(rounded, "tp", axis=1, tiled=True)

        gate_a = fold(pre_gain_first, gate_first)
        up_a = fold(pre_gain_first, up_first)
        down_a = gather(down_first)
        gate_b = fold(pre_gain_second, gate_second)
        up_b = fold(pre_gain_second, up_second)
        down_b = gather(down_second)
        middle = half_step(prompt_rows, gate_a, up_a, down_a, post_gain_first, nfs)
        result = half_step(middle, gate_b, up_b, down_b, post_gain_second, nfs)
        return (result, gate_a, up_a, down_a, gate_b, up_b, down_b)

    return jax.shard_map(
        per_device,
        mesh=mesh,
        in_specs=(P("tp", None),) + (P("fs", "tp"),) * 6 + (P(),) * 4,
        out_specs=(
            P("tp", None),
            P(None, "fs"),
            P(None, "fs"),
            P("fs", None),
            P(None, "fs"),
            P(None, "fs"),
            P("fs", None),
        ),
        check_vma=False,
    )
```
